32 devices in a mesh: ep: 4 (over y, x), tp: 8 (over z, core).
Axes of the slice: x: 2, y: 2, z: 4, core: 2. Of those that a mesh axis runs over, the one named last changes fastest.
Arguments:
- hidden: bfloat16 [64, 2048], P('ep'), may hold values from -6 to 6
- attn_gain: float32 [2048], replicated, may hold values from 0.1 to 1.9
- query_weight: bfloat16 [2048, 1024], P(None, 'tp'), may hold values from -0.125 to 0.125
- rotary_weight: bfloat16 [2048, 512], P(None, 'tp'), may hold values from -0.125 to 0.125
- key_up: bfloat16 [16, 64, 512], P('tp'), may hold values from -0.75 to 0.75
- cache_latent: bfloat16 [64, 4096, 512], P(('ep', 'tp'))
- cache_rotary: bfloat16 [64, 32, 4096], P(('ep', 'tp')), may hold values from -6 to 6
- lengths: int32 [64], P(('ep', 'tp')), may hold values from 1 to 4096, as said below
- value_up: bfloat16 [16, 512, 64], P('tp'), may hold values from -0.25 to 0.25
- out_weight: bfloat16 [1024, 2048], P('tp'), may hold values from -0.1875 to 0.1875
- mixed_gain: float32 [2048], replicated, may hold values from 0.1 to 1.9
- moe_gain: float32 [2048], replicated, may hold values from 0.1 to 1.9
- expert_ids: int32 [64, 2], replicated, may hold values from 0 to 3, all different within a row; in each aligned block of 16 rows (0 to 15, 16 to 31, ...) at most 16 rows name the same one
- route_logits: float32 [64, 2], replicated, may hold values from -6 to 6
- gate_weight: bfloat16 [4, 2048, 7168], P('ep', None, 'tp'), may hold values from -0.125 to 0.125
- up_weight: bfloat16 [4, 2048, 7168], P('ep', None, 'tp'), may hold values from -0.125 to 0.125
- down_weight: bfloat16 [4, 7168, 2048], P('ep', 'tp'), may hold values from -0.0625 to 0.0625
- final_gain: float32 [2048], replicated, may hold values from 0.1 to 1.9
Outputs:
- layer_out: bfloat16 [64, 2048], P(('ep', 'tp'))
The draws below stay inside these ranges and needn't reach their ends.
Inputs may be any that keep to these rules, and one draw needn't show every extreme that they name: `lengths`: some sequence has exactly 4096 filled positions. `expert_ids`: within each aligned block of 16 rows no expert is named more than 16 times, a bound that some block reaches.
All inputs are finite; a program needn't handle non-finite values.
Results may differ from the reference program's by a relative error of at most 0.023.
The reference program's roundings to bfloat16 on the way count: a program that leaves them out, or rounds other values in their place, can miss the bound.
Values may be sent and summed in bfloat16 or wider, within the bound.
A program may use at most 64 MiB of HBM per device.

```python
import math
import jax
import jax.numpy as jnp
import numpy as np
from jax import lax

D = 2048
HEADS = 16
NOPE = 64
ROPE = 32
VDIM = 64
LATENT = 512
EXPERT_FF = 7168
TOPK = 2
CACHE = 4096
SEQ_GROUP = 16
SEQS = 64
EXPERTS = 4
CAP = 16
N_EP = 4


def draw_cache_latent(key, part):
    normal_key = jax.random.fold_in(jax.random.fold_in(key, 11), 0)
    values = jax.random.normal(normal_key, (SEQS, CACHE, LATENT), jnp.float32)
    return values.astype(jnp.bfloat16)


def draw_lengths(key, part):
    first_key, second_key, pick_key = jax.random.split(jax.random.fold_in(key, 23), 3)
    first_draw = jax.random.randint(first_key, (SEQS,), 0, CACHE)
    second_draw = jax.random.randint(second_key, (SEQS,), 0, CACHE)
    filled = 1 + first_draw * second_draw // CACHE
    chosen_row = jax.random.randint(pick_key, (), 0, SEQS)
    return filled.at[chosen_row].set(CACHE).astype(jnp.int32)


def shard_levels(rng, dims, pieces, smallest, high):
    def one(axis_at, blocks):
        steps = jax.random.uniform(jax.random.fold_in(jax.random.fold_in(rng, 6), axis_at), (blocks,), jnp.float32, smallest / len(pieces), high / len(pieces))
        return jnp.repeat(jnp.exp(steps), dims[axis_at] // blocks).reshape((-1,) + (1,) * (len(dims) - axis_at - 1))

    gain = one(*pieces[0])
    for cut in pieces[1:]:
        gain = gain * one(*cut)
    return gain


def shared_out(stream_key, own, number, rows, count, top, most, slope):
    ranking = jax.random.permutation(stream_key, count)
    crowded, ordinary = load_shares(count, rows * top, most, slope, True), load_shares(count, rows * top, most, slope, False)
    places = jnp.arange(count)

    def named(sizes, turn):
        used = int((sizes > 0).sum())
        fixed = max(1, used // 4)
        shifted = fixed + (places - fixed + turn * (used - fixed)) % max(1, count - fixed)
        return jnp.zeros((count,), jnp.int32).at[ranking[jnp.where(places < fixed, places, shifted)]].set(jnp.asarray(sizes, jnp.int32))

    sizes = jnp.where(number % 4 == 0, named(crowded, number // 4), named(ordinary, number - number // 4 - 1))
    mixed = jax.random.permutation(jax.random.fold_in(own, 3), count)
    donor, receiver = mixed[0:count // 2 * 2:2], mixed[1:count // 2 * 2:2]
    slack = jnp.minimum(sizes[donor] - 1, most - sizes[receiver]) // 2
    slack = jnp.where((donor == ranking[0]) | (receiver == ranking[0]) | (sizes[receiver] == 0), 0, jnp.maximum(slack, 0))
    shifted = jax.random.randint(jax.random.fold_in(own, 4), (count // 2,), 0, 1 << 20) % (slack + 1)
    sizes = sizes.at[donor].add(-shifted).at[receiver].add(shifted)
    labels = jnp.searchsorted(jnp.cumsum(sizes), jnp.arange(rows * top), side="right").astype(jnp.int32)
    table = labels.reshape(top, rows).T
    table = table[jax.random.permutation(jax.random.fold_in(own, 1), rows)]
    turn = jax.random.randint(jax.random.fold_in(own, 2), (rows, 1), 0, top)
    return jnp.take_along_axis(table, (jnp.arange(top)[None, :] + turn) % top, axis=1)


def load_shares(count, total, reach, lean, full):
    portions = [(1 << 20) // math.isqrt(grade ** lean) + 1 for grade in range(1, count + 1)]
    largest = reach if full else min(reach, max(-(-total // count), total * portions[0] // sum(portions)))
    least = 1 if total - largest >= count - 1 else 0
    counts, spare = [largest] + [least] * (count - 1), total - largest - least * (count - 1)
    while spare > 0:
        free = [i for i in range(1, count) if counts[i] < largest] or [i for i in range(1, count) if counts[i] < reach]
        pool, left = sum([portions[i] for i in free]), spare
        for i in free:
            more = min(reach - counts[i], max(1, left * portions[i] // pool), spare)
            counts[i] = counts[i] + more
            spare = spare - more
    return np.array(counts)


def bell_draw(rng, shape, scale, bound, pieces=(), held_as=jnp.bfloat16):
    level = shard_levels(rng, shape, pieces, -0.22, 0.18) if pieces else 1.0
    drawn = jax.random.normal(rng, shape, jnp.float32) * scale * level
    return jnp.minimum(jnp.maximum(drawn, -bound), bound).astype(held_as)


def setup_inputs(seed: int = 0) -> dict:
    streams_of = jax.random.split(jax.random.key(seed), 19)
    hidden = bell_draw(streams_of[0], (SEQS, D), 1.0, 6.0, ((0, 4),))
    attn_gain = jnp.clip(1.0 + 0.18 * jax.random.normal(streams_of[1], (D,), jnp.float32), 0.1, 1.9)
    query_weight = bell_draw(streams_of[2], (D, HEADS * NOPE), D ** -0.5, 0.125, ((1, 8),))
    rotary_weight = bell_draw(streams_of[3], (D, HEADS * ROPE), D ** -0.5, 0.125, ((1, 8),))
    key_up = bell_draw(streams_of[4], (HEADS, NOPE, LATENT), NOPE ** -0.5, 0.75, ((0, 8),))
    cache_latent = draw_cache_latent(jax.random.fold_in(streams_of[18], 71), 0)
    cache_rotary = bell_draw(streams_of[6], (SEQS, ROPE, CACHE), 1.0, 6.0, ((0, 32),))
    lengths = draw_lengths(jax.random.fold_in(streams_of[18], 71), 0)
    value_up = bell_draw(streams_of[8], (HEADS, LATENT, VDIM), LATENT ** -0.5, 0.25, ((0, 8),))
    out_weight = bell_draw(streams_of[9], (HEADS * VDIM, D), (HEADS * VDIM) ** -0.5, 0.1875, ((0, 8),))
    mixed_gain = jnp.clip(1.0 + 0.18 * jax.random.normal(streams_of[10], (D,), jnp.float32), 0.1, 1.9)
    moe_gain = jnp.clip(1.0 + 0.18 * jax.random.normal(streams_of[11], (D,), jnp.float32), 0.1, 1.9)
    expert_ids_keys = jax.random.split(jax.random.fold_in(streams_of[12], 1), SEQS // SEQ_GROUP)
    expert_ids_turns = jax.random.permutation(jax.random.fold_in(streams_of[12], 3), SEQS // SEQ_GROUP)
    expert_ids = jax.vmap(lambda own, number: shared_out(jax.random.fold_in(streams_of[12], 2), own, number, SEQ_GROUP, EXPERTS, TOPK, CAP, 2))(expert_ids_keys, expert_ids_turns).reshape((SEQS, TOPK))
    route_logits = bell_draw(streams_of[13], (SEQS, TOPK), 1.0, 6.0, (), jnp.float32)
    gate_weight = bell_draw(streams_of[14], (EXPERTS, D, EXPERT_FF), D ** -0.5, 0.125, ((0, 4), (2, 8)))
    up_weight = bell_draw(streams_of[15], (EXPERTS, D, EXPERT_FF), D ** -0.5, 0.125, ((0, 4), (2, 8)))
    down_weight = bell_draw(streams_of[16], (EXPERTS, EXPERT_FF, D), EXPERT_FF ** -0.5, 0.0625, ((0, 4), (1, 8)))
    final_gain = jnp.clip(1.0 + 0.18 * jax.random.normal(streams_of[17], (D,), jnp.float32), 0.1, 1.9)
    return dict(hidden=hidden, attn_gain=attn_gain, query_weight=query_weight, rotary_weight=rotary_weight, key_up=key_up, cache_latent=cache_latent, cache_rotary=cache_rotary, lengths=lengths, value_up=value_up, out_weight=out_weight, mixed_gain=mixed_gain, moe_gain=moe_gain, expert_ids=expert_ids, route_logits=route_logits, gate_weight=gate_weight, up_weight=up_weight, down_weight=down_weight, final_gain=final_gain)


EPSILON = 1e-06

def norm_rows(values, gain_vector):
    values = values.astype(jnp.float32)
    factor = lax.rsqrt(lax.optimization_barrier(jnp.mean(values * values, axis=-1, keepdims=True)) + EPSILON)
    return values * factor * gain_vector

def rotate(values, position):
    half_width = values.shape[-1] // 2
    inverse = 10000.0 ** (-jnp.arange(half_width, dtype=jnp.float32) / half_width)
    angles = position.astype(jnp.float32)[:, None, None] * inverse
    cosine = jnp.cos(angles)
    sine_part = jnp.sin(angles)
    first_half = values[..., :half_width]
    second = values[..., half_width:]
    return jnp.concatenate([first_half * cosine - second * sine_part, second * cosine + first_half * sine_part], axis=-1)

def slot_tables(group_ids, group_probs, experts, capacity):
    row_count, top_count = group_ids.shape
    flat_ids = group_ids.reshape(-1)
    onehot = (flat_ids[:, None] == jnp.arange(experts, dtype=jnp.int32)[None, :]).astype(jnp.int32)
    earlier = jnp.cumsum(onehot, axis=0) - onehot
    slot_index = lax.optimization_barrier(jnp.sum(earlier * onehot, axis=1))
    target = flat_ids * capacity + slot_index
    source = jnp.arange(row_count * top_count, dtype=jnp.int32) // top_count
    slot_rows = jnp.full((experts * capacity,), row_count, jnp.int32).at[target].set(source)
    slot_gates = jnp.zeros((experts * capacity,), jnp.float32).at[target].set(group_probs.reshape(-1))
    return (slot_rows, slot_gates)

def reference(hidden, attn_gain, query_weight, rotary_weight, key_up, cache_latent, cache_rotary, lengths, value_up, out_weight, mixed_gain, moe_gain, expert_ids, route_logits, gate_weight, up_weight, down_weight, final_gain):
    normed_in = norm_rows(hidden, attn_gain).astype(jnp.bfloat16)
    query_nope = jnp.dot(normed_in, query_weight, preferred_element_type=jnp.float32).astype(jnp.bfloat16)
    query_nope = query_nope.reshape(SEQS, HEADS, NOPE)
    query_pe = jnp.dot(normed_in, rotary_weight, preferred_element_type=jnp.float32).astype(jnp.bfloat16)
    query_pe = query_pe.reshape(SEQS, HEADS, ROPE)
    query_latent = jnp.einsum('shn,hnc->shc', query_nope.astype(jnp.float32), key_up.astype(jnp.float32)).astype(jnp.bfloat16)
    query_rot = rotate(query_pe.astype(jnp.float32), lengths - 1).astype(jnp.bfloat16)
    score_scale = (NOPE + ROPE) ** (-0.5)

    def attend_one(operands):
        latent_query, rotary_query, latent, rope_keys, length = operands
        scores = jnp.dot(latent_query, latent.T, preferred_element_type=jnp.float32)
        scores = (scores + jnp.dot(rotary_query, rope_keys, preferred_element_type=jnp.float32)) * score_scale
        visible = jnp.arange(CACHE, dtype=jnp.int32)[None, :] < length
        scores = jnp.where(visible, scores, -jnp.inf)
        highest = lax.optimization_barrier(jnp.max(scores, axis=-1, keepdims=True))
        weights = jnp.exp(scores - highest)
        probs = (weights / lax.optimization_barrier(jnp.sum(weights, axis=-1, keepdims=True))).astype(jnp.bfloat16)
        return jnp.dot(probs, latent, preferred_element_type=jnp.float32).astype(jnp.bfloat16)
    out_latent = lax.map(attend_one, (query_latent, query_rot, cache_latent, cache_rotary, lengths))
    head_out = jnp.einsum('shc,hcv->shv', out_latent.astype(jnp.float32), value_up.astype(jnp.float32)).astype(jnp.bfloat16)
    attended = jnp.dot(head_out.reshape(SEQS, HEADS * VDIM), out_weight, preferred_element_type=jnp.float32).astype(jnp.bfloat16)
    mixed_rows = (hidden.astype(jnp.float32) + norm_rows(attended, mixed_gain)).astype(jnp.bfloat16)
    normed = norm_rows(mixed_rows, moe_gain).astype(jnp.bfloat16)
    gate_probs = jax.nn.softmax(route_logits.astype(jnp.float32), axis=-1)

    def tables_for(group_ids, group_probs):
        return slot_tables(group_ids, group_probs, EXPERTS, CAP)
    slot_rows, slot_gates = jax.vmap(tables_for)(expert_ids.reshape(N_EP, SEQ_GROUP, TOPK), gate_probs.reshape(N_EP, SEQ_GROUP, TOPK))
    offsets = jnp.arange(N_EP, dtype=jnp.int32)[:, None] * SEQ_GROUP
    global_rows = jnp.where(slot_rows < SEQ_GROUP, slot_rows + offsets, SEQS)
    global_rows = global_rows.reshape(N_EP, EXPERTS, CAP).transpose(1, 0, 2).reshape(EXPERTS, N_EP * CAP)
    expert_gates = slot_gates.reshape(N_EP, EXPERTS, CAP).transpose(1, 0, 2).reshape(EXPERTS, N_EP * CAP)
    padded = jnp.concatenate([normed, jnp.zeros((1, D), jnp.bfloat16)], axis=0)

    def one_expert(operands):
        row_index, gate_matrix, up_matrix, down_matrix = operands
        picked = padded[row_index]
        gate_part = jnp.dot(picked, gate_matrix, preferred_element_type=jnp.float32)
        up_part = jnp.dot(picked, up_matrix, preferred_element_type=jnp.float32)
        act = (jax.nn.silu(gate_part) * up_part).astype(jnp.bfloat16)
        return jnp.dot(act, down_matrix, preferred_element_type=jnp.float32)
    expert_out = lax.map(one_expert, (global_rows, gate_weight, up_weight, down_weight))
    weighted = expert_out.reshape(EXPERTS * N_EP * CAP, D) * expert_gates.reshape(-1)[:, None]
    combined = jnp.zeros((SEQS + 1, D), jnp.float32).at[global_rows.reshape(-1)].add(weighted)
    routed = combined[:SEQS].astype(jnp.bfloat16)
    return (mixed_rows.astype(jnp.float32) + norm_rows(routed, final_gain)).astype(jnp.bfloat16)
```

```python
import functools

import jax
import jax.numpy as jnp
import numpy as np
from jax import lax
from jax.experimental import pallas as pl
from jax.experimental.pallas import tpu as pltpu
from jax.sharding import PartitionSpec as P

EPSILON = 1e-06
F32 = jnp.float32
BF16 = jnp.bfloat16
MESH = pl.DeviceIdType.MESH


def rms(values, gain):
    factor = lax.rsqrt(jnp.mean(values * values, axis=-1, keepdims=True) + EPSILON)
    return values * factor * gain


def dot(a, b):
    return jnp.dot(a, b, preferred_element_type=F32)


def iota(shape, dim):
    return lax.broadcasted_iota(jnp.int32, shape, dim)


def kernel(
    dims,
    lengths,
    inverse,
    hidden_h,
    attn_gain_h,
    query_weight_h,
    rotary_weight_h,
    key_up_h,
    cache_rotary_h,
    cache_latent_h,
    value_up_h,
    out_weight_h,
    mixed_gain_h,
    moe_gain_h,
    expert_ids_h,
    logits_h,
    gate_weight_h,
    up_weight_h,
    down_weight_h,
    final_gain_h,
    out_ref,
    inverse_v,
    hidden,
    attn_gain,
    query_weight,
    rotary_weight,
    key_up,
    cache_rotary,
    cache_latent,
    value_up,
    out_weight,
    mixed_gain,
    moe_gain,
    expert_ids,
    logits,
    gate_weight,
    up_weight,
    down_weight,
    final_gain,
    q_stage,
    q_send,
    q_recv,
    q_rows,
    score_buf,
    o_stage,
    o_send,
    o_recv,
    o_rows,
    a_stage,
    a_send,
    a_recv,
    n_send,
    n_recv,
    x_stage,
    x_rows,
    act_buf,
    y_stage,
    y_send,
    y_recv,
    local_sem,
    send_sem,
    recv_sem,
):
    E, T, lh, nope, rope, own = dims
    N = E * T
    H = T * lh
    rows, features = hidden.shape
    latent = key_up.shape[1]
    cache_len = cache_latent.shape[1]
    all_rows = x_rows.shape[0]
    me_e = lax.axis_index("ep")
    me_t = lax.axis_index("tp")
    me = me_e * T + me_t

    pairs = [
        (hidden_h, hidden),
        (attn_gain_h, attn_gain),
        (query_weight_h, query_weight),
        (rotary_weight_h, rotary_weight),
        (key_up_h, key_up),
        (inverse, inverse_v),
        (cache_rotary_h, cache_rotary),
    ]
    cache_at = len(pairs)
    pairs += [(cache_latent_h.at[s], cache_latent.at[s]) for s in range(own)]
    rest_at = len(pairs)
    pairs += [
        (value_up_h, value_up),
        (out_weight_h, out_weight),
        (mixed_gain_h, mixed_gain),
        (moe_gain_h, moe_gain),
        (expert_ids_h, expert_ids),
        (logits_h, logits),
        (final_gain_h, final_gain),
    ]
    expert_at = len(pairs)
    pairs += [
        (gate_weight_h, gate_weight),
        (up_weight_h, up_weight),
        (down_weight_h, down_weight),
    ]
    copies = [
        pltpu.make_async_copy(src, dst, local_sem.at[i]) for i, (src, dst) in enumerate(pairs)
    ]
    for c in copies:
        c.start()

    barrier = pltpu.get_barrier_semaphore()

    def greet(i, carry):
        p = lax.rem(me + i, N)
        pl.semaphore_signal(
            barrier,
            inc=1,
            device_id={"ep": p // T, "tp": lax.rem(p, T)},
            device_id_type=MESH,
        )
        return carry

    lax.fori_loop(1, N, greet, 0)

    def tp_send(send, recv, k):
        def one(i, carry):
            p = lax.rem(me_t + i, T)
            pltpu.make_async_remote_copy(
                src_ref=send.at[p],
                dst_ref=recv.at[me_t],
                send_sem=send_sem.at[k],
                recv_sem=recv_sem.at[k],
                device_id={"tp": p},
                device_id_type=MESH,
            ).start()
            return carry

        lax.fori_loop(1, T, one, 0)

    def all_send(source, recv, k):
        def one(i, carry):
            p = lax.rem(me + i, N)
            pltpu.make_async_remote_copy(
                src_ref=source(p),
                dst_ref=recv.at[me],
                send_sem=send_sem.at[k],
                recv_sem=recv_sem.at[k],
                device_id={"ep": p // T, "tp": lax.rem(p, T)},
                device_id_type=MESH,
            ).start()
            return carry

        lax.fori_loop(1, N, one, 0)

    def await_bytes(buffer, sem, count):
        part = buffer.at[pl.ds(0, count)]
        pltpu.make_async_copy(part, part, sem).wait()

    for c in copies[:cache_at - 2]:
        c.wait()
    hid = hidden[...].astype(F32)
    normed_in = rms(hid, attn_gain[...]).astype(BF16)
    q_nope = dot(normed_in, query_weight[...]).astype(BF16)
    q_pe = dot(normed_in, rotary_weight[...]).astype(BF16)
    nope_head = iota(q_nope.shape, 1) // nope
    pe_head = iota(q_pe.shape, 1) // rope
    fold = (
        lax.rem(iota((lh * rope, rope), 0), rope) == iota((lh * rope, rope), 1)
    ).astype(BF16)
    q_stage[...] = jnp.zeros_like(q_stage)
    for h in range(lh):
        q_h = jnp.where(nope_head == h, q_nope, jnp.zeros_like(q_nope))
        q_stage[h, :, 0:latent] = dot(q_h, key_up[...])
        pe_h = jnp.where(pe_head == h, q_pe, jnp.zeros_like(q_pe))
        q_stage[h, :, latent:latent + rope] = dot(pe_h, fold)
    for j in range(T):
        for h in range(lh):
            q_send[j, h] = q_stage[h, own * j:own * (j + 1), :].astype(BF16)
    pl.semaphore_wait(barrier, N - 1)
    tp_send(q_send, q_recv, 0)
    q_recv[me_t] = q_send[me_t]

    inv = copies[cache_at - 2]
    inv.wait()
    copies[cache_at - 1].wait()
    await_bytes(q_recv, recv_sem.at[0], T - 1)
    for t in range(T):
        for h in range(lh):
            got = q_recv[t, h].astype(F32)
            at = t * lh + h
            for s in range(own):
                q_rows[s, at:at + 1, :] = got[s:s + 1, :]

    half = rope // 2
    turn_row = iota((rope, rope), 0)
    turn_col = iota((rope, rope), 1)
    turn = jnp.where(
        turn_row == turn_col + half,
        -1.0,
        jnp.where(turn_row == turn_col - half, 1.0, 0.0),
    ).astype(BF16)
    scale = (nope + rope) ** (-0.5)
    chunk = min(1024, cache_len)
    for s in range(own):
        length = lengths[s]
        angles = (length - 1).astype(F32) * inverse_v[...]
        pe = q_rows[s, :, latent:latent + rope]
        rot = (pe * jnp.cos(angles) + dot(pe.astype(BF16), turn) * jnp.sin(angles)).astype(BF16)
        lat = q_rows[s, :, 0:latent].astype(BF16)
        copies[cache_at + s].wait()
        for c in range(0, cache_len, chunk):
            part = lax.dot_general(
                lat,
                cache_latent[s, c:c + chunk, :],
                (((1,), (1,)), ((), ())),
                preferred_element_type=F32,
            )
            part = part + dot(rot, cache_rotary[s, :, c:c + chunk])
            seen = iota(part.shape, 1) + c < length
            score_buf[:, c:c + chunk] = jnp.where(seen, part * scale, -jnp.inf)
        highest = jnp.max(score_buf[...], axis=-1, keepdims=True)
        weights = jnp.exp(score_buf[...] - highest)
        total = jnp.sum(weights, axis=-1, keepdims=True)
        probs = (weights / total).astype(BF16)
        acc = jnp.zeros((H, latent), F32)
        for c in range(0, cache_len, chunk):
            acc = acc + dot(probs[:, c:c + chunk], cache_latent[s, c:c + chunk, :])
        o_stage[s] = acc
    for t in range(T):
        for s in range(own):
            o_send[t, s] = o_stage[s, t * lh:(t + 1) * lh, :].astype(BF16)
    tp_send(o_send, o_recv, 1)
    o_recv[me_t] = o_send[me_t]
    for c in copies[rest_at:expert_at]:
        c.wait()
    gate_probs = jax.nn.softmax(logits[...], axis=-1)
    row_gates = jnp.sum(
        jnp.where(expert_ids[...] == me_e, gate_probs, 0.0), axis=-1, keepdims=True
    )
    pick = (iota((own, rows), 1) == iota((own, rows), 0) + me_t * own).astype(BF16)
    hidden_own = dot(pick, hidden[...])

    await_bytes(o_recv, recv_sem.at[1], T - 1)
    for j in range(T):
        for s in range(own):
            got = o_recv[j, s].astype(F32)
            at = j * own + s
            for h in range(lh):
                o_rows[h, at:at + 1, :] = got[h:h + 1, :]
    terms = jnp.zeros((rows, features), F32)
    for h in range(lh):
        o_h = o_rows[h].astype(BF16)
        head_out = dot(o_h, value_up[h]).astype(BF16)
        width = head_out.shape[1]
        terms = terms + dot(head_out, out_weight[h * width:(h + 1) * width, :])
    a_stage[...] = terms
    for j in range(T):
        a_send[j] = a_stage[own * j:own * (j + 1), :].astype(BF16)
    tp_send(a_send, a_recv, 2)
    a_recv[me_t] = a_send[me_t]
    await_bytes(a_recv, recv_sem.at[2], T - 1)
    attended = jnp.zeros((own, features), F32)
    for j in range(T):
        attended = attended + a_recv[j].astype(F32)
    attended = attended.astype(BF16).astype(F32)
    mixed = (hidden_own + rms(attended, mixed_gain[...])).astype(BF16).astype(F32)
    n_send[0] = rms(mixed, moe_gain[...]).astype(BF16)

    all_send(lambda p: n_send.at[0], n_recv, 3)
    n_recv[me] = n_send[0]
    for c in copies[expert_at:]:
        c.wait()
    await_bytes(n_recv, recv_sem.at[3], N - 1)
    for j in range(N):
        x_stage[own * j:own * (j + 1), :] = n_recv[j].astype(F32)
    x_rows[...] = x_stage[...].astype(BF16)
    block = min(64, all_rows)
    step = min(512, features)

    def run_block(b, carry):
        at = pl.ds(pl.multiple_of(b * block, block), block)
        picked = x_rows[at, :]
        gate_part = dot(picked, gate_weight[0])
        up_part = dot(picked, up_weight[0])
        act_buf[at, :] = (gate_part / (1.0 + jnp.exp(-gate_part)) * up_part).astype(BF16)
        for c in range(0, features, step):
            y_stage[at, c:c + step] = dot(act_buf[at, :], down_weight[0, :, c:c + step])
        return carry

    if block == all_rows:
        run_block(0, 0)
    else:
        lax.fori_loop(0, all_rows // block, run_block, 0)
    y_stage[...] = y_stage[...] * row_gates
    for j in range(N):
        y_send[j] = y_stage[own * j:own * (j + 1), :].astype(BF16)
    all_send(lambda p: y_send.at[p], y_recv, 4)
    y_recv[me] = y_send[me]
    await_bytes(y_recv, recv_sem.at[4], N - 1)

    def add(j, acc):
        return acc + y_recv[j].astype(F32)

    routed = lax.fori_loop(0, N, add, jnp.zeros((own, features), F32), unroll=8)
    routed = routed.astype(BF16).astype(F32)
    out_ref[...] = (mixed + rms(routed, final_gain[...])).astype(BF16)

    await_bytes(q_send, send_sem.at[0], T - 1)
    await_bytes(o_send, send_sem.at[1], T - 1)
    await_bytes(a_send, send_sem.at[2], T - 1)
    await_bytes(n_recv, send_sem.at[3], N - 1)
    await_bytes(y_send, send_sem.at[4], N - 1)


def body(
    hidden,
    attn_gain,
    query_weight,
    rotary_weight,
    key_up,
    cache_latent,
    cache_rotary,
    lengths,
    value_up,
    out_weight,
    mixed_gain,
    moe_gain,
    expert_ids,
    route_logits,
    gate_weight,
    up_weight,
    down_weight,
    final_gain,
):
    E, T = lax.axis_size("ep"), lax.axis_size("tp")
    N = E * T
    rows, features = hidden.shape
    lh, nope, latent = key_up.shape
    rope = rotary_weight.shape[1] // lh
    own, cache_len, _ = cache_latent.shape
    H = T * lh
    all_rows = expert_ids.shape[0]
    ff = gate_weight.shape[2]
    wide = latent + 128
    freq = (10000.0 ** (-np.arange(rope // 2, dtype=np.float32) / (rope // 2))).astype(np.float32)
    inverse = jnp.asarray(np.concatenate([freq, freq])[None, :])
    arrays = [
        inverse,
        hidden,
        attn_gain.reshape(1, -1),
        query_weight,
        rotary_weight,
        key_up.reshape(lh * nope, latent),
        cache_rotary,
        cache_latent,
        value_up,
        out_weight,
        mixed_gain.reshape(1, -1),
        moe_gain.reshape(1, -1),
        expert_ids,
        route_logits,
        gate_weight,
        up_weight,
        down_weight,
        final_gain.reshape(1, -1),
    ]
    anywhere = pl.BlockSpec(memory_space=pl.ANY)
    v = pltpu.VMEM
    n_copies = len(arrays) - 1 + own
    scratch = [v(a.shape, a.dtype) for a in arrays] + [
        v((lh, rows, wide), F32),
        v((T, lh, own, wide), BF16),
        v((T, lh, own, wide), BF16),
        v((own, H, wide), F32),
        v((H, cache_len), F32),
        v((own, H, latent), F32),
        v((T, own, lh, latent), BF16),
        v((T, own, lh, latent), BF16),
        v((lh, rows, latent), F32),
        v((rows, features), F32),
        v((T, own, features), BF16),
        v((T, own, features), BF16),
        v((1, own, features), BF16),
        v((N, own, features), BF16),
        v((all_rows, features), F32),
        v((all_rows, features), BF16),
        v((all_rows, ff), BF16),
        v((all_rows, features), F32),
        v((N, own, features), BF16),
        v((N, own, features), BF16),
        pltpu.SemaphoreType.DMA((n_copies,)),
        pltpu.SemaphoreType.DMA((5,)),
        pltpu.SemaphoreType.DMA((5,)),
    ]
    return pl.pallas_call(
        functools.partial(kernel, (E, T, lh, nope, rope, own)),
        out_shape=jax.ShapeDtypeStruct((own, features), BF16),
        in_specs=[pl.BlockSpec(memory_space=pltpu.SMEM)] + [anywhere] * len(arrays),
        out_specs=pl.BlockSpec(memory_space=pltpu.VMEM),
        scratch_shapes=scratch,
        compiler_params=pltpu.CompilerParams(
            collective_id=0,
            has_side_effects=True,
            vmem_limit_bytes=62 * 1024 * 1024,
        ),
    )(lengths, *arrays)


def solution(mesh):
    placed = (
        P("ep", None),
        P(),
        P(None, "tp"),
        P(None, "tp"),
        P("tp", None, None),
        P(("ep", "tp"), None, None),
        P(("ep", "tp"), None, None),
        P(("ep", "tp")),
        P("tp", None, None),
        P("tp", None),
        P(),
        P(),
        P(),
        P(),
        P("ep", None, "tp"),
        P("ep", None, "tp"),
        P("ep", "tp", None),
        P(),
    )
    return jax.shard_map(
        body, mesh=mesh, in_specs=placed, out_specs=P(("ep", "tp"), None), check_vma=False
    )
```

```python
import functools

import jax
import jax.numpy as jnp
import numpy as np
from jax import lax
from jax.experimental import pallas as pl
from jax.experimental.pallas import tpu as pltpu
from jax.sharding import PartitionSpec as P

EPSILON = 1e-06
F32 = jnp.float32
BF16 = jnp.bfloat16
MESH = pl.DeviceIdType.MESH


def rms(values, gain):
    factor = lax.rsqrt(jnp.mean(values * values, axis=-1, keepdims=True) + EPSILON)
    return values * factor * gain


def dot(a, b):
    return jnp.dot(a, b, preferred_element_type=F32)


def dot_t(a, b):
    return lax.dot_general(a, b, (((1,), (1,)), ((), ())), preferred_element_type=F32)


def iota(shape, dim):
    return lax.broadcasted_iota(jnp.int32, shape, dim)


def kernel(
    dims,
    lengths,
    inverse,
    hidden_h,
    attn_gain_h,
    query_weight_h,
    rotary_weight_h,
    key_up_h,
    cache_rotary_h,
    cache_latent_h,
    value_up_h,
    out_weight_h,
    mixed_gain_h,
    moe_gain_h,
    expert_ids_h,
    logits_h,
    gate_weight_h,
    up_weight_h,
    down_weight_h,
    final_gain_h,
    out_ref,
    inverse_v,
    hidden,
    attn_gain,
    query_weight,
    rotary_weight,
    key_up,
    cache_rotary,
    cache_latent,
    value_up,
    out_weight,
    mixed_gain,
    moe_gain,
    expert_ids,
    logits,
    gate_weight,
    up_weight,
    down_weight,
    final_gain,
    q_stage,
    q_send,
    q_recv,
    q_rows,
    score_buf,
    o_stage,
    o_send,
    o_recv,
    o_rows,
    a_stage,
    a_send,
    a_recv,
    n_send,
    n_recv,
    x_rows,
    act_buf,
    y_stage,
    y_send,
    y_recv,
    local_sem,
    send_sem,
    recv_sem,
    chip_sem,
):
    E, T, lh, nope, rope, own = dims
    N = E * T
    H = T * lh
    rows, features = hidden.shape
    latent = key_up.shape[1]
    cache_len = cache_latent.shape[1]
    all_rows = x_rows.shape[0]
    me_e = lax.axis_index("ep")
    me_t = lax.axis_index("tp")
    me = me_e * T + me_t

    pairs = [
        (hidden_h, hidden),
        (attn_gain_h, attn_gain),
        (query_weight_h, query_weight),
        (rotary_weight_h, rotary_weight),
        (key_up_h, key_up),
        (inverse, inverse_v),
        (cache_rotary_h, cache_rotary),
    ]
    cache_at = len(pairs)
    pairs += [(cache_latent_h.at[s], cache_latent.at[s]) for s in range(own)]
    rest_at = len(pairs)
    pairs += [
        (value_up_h, value_up),
        (out_weight_h, out_weight),
        (mixed_gain_h, mixed_gain),
        (moe_gain_h, moe_gain),
        (expert_ids_h, expert_ids),
        (logits_h, logits),
        (final_gain_h, final_gain),
    ]
    expert_at = len(pairs)
    pairs += [
        (gate_weight_h, gate_weight),
        (up_weight_h, up_weight),
        (down_weight_h, down_weight),
    ]
    copies = [
        pltpu.make_async_copy(src, dst, local_sem.at[i]) for i, (src, dst) in enumerate(pairs)
    ]
    for c in copies:
        c.start()

    barrier = pltpu.get_barrier_semaphore()

    def greet(i, carry):
        p = lax.rem(me + i, N)
        pl.semaphore_signal(
            barrier,
            inc=1,
            device_id={"ep": p // T, "tp": lax.rem(p, T)},
            device_id_type=MESH,
        )
        return carry

    lax.fori_loop(1, N, greet, 0)

    def tp_send(send, recv, k):
        def one(i, carry):
            p = lax.rem(me_t + i, T)
            pltpu.make_async_remote_copy(
                src_ref=send.at[p],
                dst_ref=recv.at[me_t],
                send_sem=send_sem.at[k],
                recv_sem=recv_sem.at[k],
                device_id={"tp": p},
                device_id_type=MESH,
            ).start()
            return carry

        lax.fori_loop(1, T, one, 0)

    def all_send(source, recv, k):
        def one(i, carry):
            p = lax.rem(me + i, N)
            pltpu.make_async_remote_copy(
                src_ref=source(p),
                dst_ref=recv.at[me],
                send_sem=send_sem.at[k],
                recv_sem=recv_sem.at[k],
                device_id={"ep": p // T, "tp": lax.rem(p, T)},
                device_id_type=MESH,
            ).start()
            return carry

        lax.fori_loop(1, N, one, 0)

    def await_bytes(buffer, sem, count):
        part = buffer.at[pl.ds(0, count)]
        pltpu.make_async_copy(part, part, sem).wait()

    for c in copies[:cache_at - 2]:
        c.wait()
    hid = hidden[...].astype(F32)
    normed_in = rms(hid, attn_gain[...]).astype(BF16)
    q_nope = dot(normed_in, query_weight[...]).astype(BF16)
    q_pe = dot_t(normed_in, rotary_weight[...]).astype(BF16)
    nope_head = iota(q_nope.shape, 1) // nope
    pe_head = iota(q_pe.shape, 1) // rope
    fold = (
        lax.rem(iota((lh * rope, rope), 0), rope) == iota((lh * rope, rope), 1)
    ).astype(BF16)
    q_stage[...] = jnp.zeros_like(q_stage)
    for h in range(lh):
        q_h = jnp.where(nope_head == h, q_nope, jnp.zeros_like(q_nope))
        q_stage[h, :, 0:latent] = dot(q_h, key_up[...])
        pe_h = jnp.where(pe_head == h, q_pe, jnp.zeros_like(q_pe))
        q_stage[h, :, latent:latent + rope] = dot(pe_h, fold)
    for j in range(T):
        for h in range(lh):
            q_send[j, h] = q_stage[h, own * j:own * (j + 1), :].astype(BF16)
    pl.semaphore_wait(barrier, N - 1)
    tp_send(q_send, q_recv, 0)
    q_recv[me_t] = q_send[me_t]

    inv = copies[cache_at - 2]
    inv.wait()
    copies[cache_at - 1].wait()
    await_bytes(q_recv, recv_sem.at[0], T - 1)
    for t in range(T):
        for h in range(lh):
            got = q_recv[t, h].astype(F32)
            at = t * lh + h
            for s in range(own):
                q_rows[s, at:at + 1, :] = got[s:s + 1, :]

    half = rope // 2
    turn_row = iota((rope, rope), 0)
    turn_col = iota((rope, rope), 1)
    turn = jnp.where(
        turn_row == turn_col + half,
        -1.0,
        jnp.where(turn_row == turn_col - half, 1.0, 0.0),
    ).astype(BF16)
    scale = (nope + rope) ** (-0.5)
    chunk = min(1024, cache_len)
    for s in range(own):
        length = lengths[s]
        angles = (length - 1).astype(F32) * inverse_v[...]
        pe = q_rows[s, :, latent:latent + rope]
        rot = (pe * jnp.cos(angles) + dot(pe.astype(BF16), turn) * jnp.sin(angles)).astype(BF16)
        lat = q_rows[s, :, 0:latent].astype(BF16)
        copies[cache_at + s].wait()
        for c in range(0, cache_len, chunk):
            part = dot_t(lat, cache_latent[s, c:c + chunk, :])
            part = part + dot(rot, cache_rotary[s, :, c:c + chunk])
            seen = iota(part.shape, 1) + c < length
            score_buf[:, c:c + chunk] = jnp.where(seen, part * scale, -jnp.inf)
        highest = jnp.max(score_buf[...], axis=-1, keepdims=True)
        weights = jnp.exp(score_buf[...] - highest)
        total = jnp.sum(weights, axis=-1, keepdims=True)
        probs = (weights / total).astype(BF16)
        acc = jnp.zeros((H, latent), F32)
        for c in range(0, cache_len, chunk):
            acc = acc + dot(probs[:, c:c + chunk], cache_latent[s, c:c + chunk, :])
        o_stage[s] = acc
    for t in range(T):
        for s in range(own):
            o_send[t, s] = o_stage[s, t * lh:(t + 1) * lh, :].astype(BF16)
    tp_send(o_send, o_recv, 1)
    o_recv[me_t] = o_send[me_t]
    for c in copies[rest_at:expert_at]:
        c.wait()
    gate_probs = jax.nn.softmax(logits[...], axis=0)
    gate_line = jnp.sum(
        jnp.where(expert_ids[...] == me_e, gate_probs, 0.0), axis=0, keepdims=True
    )
    square = (all_rows, all_rows)
    row_gates = jnp.sum(
        jnp.where(iota(square, 0) == iota(square, 1), gate_line, 0.0), axis=-1, keepdims=True
    )
    pick = (iota((own, rows), 1) == iota((own, rows), 0) + me_t * own).astype(BF16)
    hidden_own = dot(pick, hidden[...])

    await_bytes(o_recv, recv_sem.at[1], T - 1)
    for j in range(T):
        for s in range(own):
            got = o_recv[j, s].astype(F32)
            at = j * own + s
            for h in range(lh):
                o_rows[h, at:at + 1, :] = got[h:h + 1, :]
    terms = jnp.zeros((rows, features), F32)
    for h in range(lh):
        o_h = o_rows[h].astype(BF16)
        head_out = dot_t(o_h, value_up[h]).astype(BF16)
        width = head_out.shape[1]
        terms = terms + dot(head_out, out_weight[h * width:(h + 1) * width, :])
    a_stage[...] = terms
    for j in range(T):
        a_send[j] = a_stage[own * j:own * (j + 1), :].astype(BF16)
    tp_send(a_send, a_recv, 2)
    a_recv[me_t] = a_send[me_t]
    await_bytes(a_recv, recv_sem.at[2], T - 1)
    attended = jnp.zeros((own, features), F32)
    for j in range(T):
        attended = attended + a_recv[j].astype(F32)
    attended = attended.astype(BF16).astype(F32)
    mixed = (hidden_own + rms(attended, mixed_gain[...])).astype(BF16).astype(F32)
    n_send[0] = rms(mixed, moe_gain[...]).astype(BF16)

    side = lax.rem(me, 2)
    chips = N // 2

    def place(p):
        return {"ep": p // T, "tp": lax.rem(p, T)}

    def spread(source, slot, target, sem):
        pltpu.make_async_remote_copy(
            src_ref=source,
            dst_ref=n_recv.at[slot],
            send_sem=send_sem.at[3],
            recv_sem=sem,
            device_id=place(target),
            device_id_type=MESH,
        ).start()

    pair = me + 1 - 2 * side

    def outward(i, carry):
        spread(n_send.at[0], me, 2 * lax.rem(me // 2 + i, chips) + side, chip_sem.at[me // 2])
        return carry

    lax.fori_loop(1, chips, outward, 0)
    spread(n_send.at[0], me, pair, recv_sem.at[3])
    n_recv[me] = n_send[0]

    def hand_on(i, carry):
        chip = lax.rem(me // 2 + chips - i, chips)
        p = 2 * chip + side
        pltpu.make_async_copy(n_recv.at[p], n_recv.at[p], chip_sem.at[chip]).wait()
        spread(n_recv.at[p], p, pair, recv_sem.at[3])
        return carry

    lax.fori_loop(1, chips, hand_on, 0)
    for c in copies[expert_at:]:
        c.wait()
    await_bytes(n_recv, recv_sem.at[3], chips)
    for j in range(N):
        x_rows[own * j:own * (j + 1), :] = n_recv[j]
    block = min(64, all_rows)
    step = min(512, features)

    def run_block(b, carry):
        at = pl.ds(pl.multiple_of(b * block, block), block)
        picked = x_rows[at, :]
        gate_part = dot(picked, gate_weight[0])
        up_part = dot(picked, up_weight[0])
        act_buf[at, :] = (gate_part / (1.0 + jnp.exp(-gate_part)) * up_part).astype(BF16)
        for c in range(0, features, step):
            y_stage[at, c:c + step] = dot(act_buf[at, :], down_weight[0, :, c:c + step])
        return carry

    if block == all_rows:
        run_block(0, 0)
    else:
        lax.fori_loop(0, all_rows // block, run_block, 0)
    y_stage[...] = y_stage[...] * row_gates
    for j in range(N):
        y_send[j] = y_stage[own * j:own * (j + 1), :].astype(BF16)
    all_send(lambda p: y_send.at[p], y_recv, 4)
    y_recv[me] = y_send[me]
    await_bytes(y_recv, recv_sem.at[4], N - 1)

    def add(j, acc):
        return acc + y_recv[j].astype(F32)

    routed = lax.fori_loop(0, N, add, jnp.zeros((own, features), F32), unroll=8)
    routed = routed.astype(BF16).astype(F32)
    out_ref[...] = (mixed + rms(routed, final_gain[...])).astype(BF16)

    await_bytes(q_send, send_sem.at[0], T - 1)
    await_bytes(o_send, send_sem.at[1], T - 1)
    await_bytes(a_send, send_sem.at[2], T - 1)
    await_bytes(n_recv, send_sem.at[3], N - 1)
    await_bytes(y_send, send_sem.at[4], N - 1)


def body(
    hidden,
    attn_gain,
    query_weight,
    rotary_weight,
    key_up,
    cache_latent,
    cache_rotary,
    lengths,
    value_up,
    out_weight,
    mixed_gain,
    moe_gain,
    expert_ids,
    route_logits,
    gate_weight,
    up_weight,
    down_weight,
    final_gain,
):
    E, T = lax.axis_size("ep"), lax.axis_size("tp")
    N = E * T
    rows, features = hidden.shape
    lh, nope, latent = key_up.shape
    rope = rotary_weight.shape[1] // lh
    own, cache_len, _ = cache_latent.shape
    H = T * lh
    all_rows = expert_ids.shape[0]
    ff = gate_weight.shape[2]
    wide = latent + 128
    freq = (10000.0 ** (-np.arange(rope // 2, dtype=np.float32) / (rope // 2))).astype(np.float32)
    inverse = jnp.asarray(np.concatenate([freq, freq])[None, :])
    arrays = [
        inverse,
        hidden,
        attn_gain.reshape(1, -1),
        query_weight,
        rotary_weight.T,
        key_up.reshape(lh * nope, latent),
        cache_rotary,
        cache_latent,
        value_up.transpose(0, 2, 1),
        out_weight,
        mixed_gain.reshape(1, -1),
        moe_gain.reshape(1, -1),
        expert_ids.T,
        route_logits.T,
        gate_weight,
        up_weight,
        down_weight,
        final_gain.reshape(1, -1),
    ]
    anywhere = pl.BlockSpec(memory_space=pl.ANY)
    v = pltpu.VMEM
    n_copies = len(arrays) - 1 + own
    scratch = [v(a.shape, a.dtype) for a in arrays] + [
        v((lh, rows, wide), F32),
        v((T, lh, own, wide), BF16),
        v((T, lh, own, wide), BF16),
        v((own, H, wide), F32),
        v((H, cache_len), F32),
        v((own, H, latent), F32),
        v((T, own, lh, latent), BF16),
        v((T, own, lh, latent), BF16),
        v((lh, rows, latent), F32),
        v((rows, features), F32),
        v((T, own, features), BF16),
        v((T, own, features), BF16),
        v((1, own, features), BF16),
        v((N, own, features), BF16),
        v((all_rows, features), BF16),
        v((all_rows, ff), BF16),
        v((all_rows, features), F32),
        v((N, own, features), BF16),
        v((N, own, features), BF16),
        pltpu.SemaphoreType.DMA((n_copies,)),
        pltpu.SemaphoreType.DMA((5,)),
        pltpu.SemaphoreType.DMA((5,)),
        pltpu.SemaphoreType.DMA((N // 2,)),
    ]
    return pl.pallas_call(
        functools.partial(kernel, (E, T, lh, nope, rope, own)),
        out_shape=jax.ShapeDtypeStruct((own, features), BF16),
        in_specs=[pl.BlockSpec(memory_space=pltpu.SMEM)] + [anywhere] * len(arrays),
        out_specs=pl.BlockSpec(memory_space=pltpu.VMEM),
        scratch_shapes=scratch,
        compiler_params=pltpu.CompilerParams(
            collective_id=0,
            has_side_effects=True,
            vmem_limit_bytes=62 * 1024 * 1024,
        ),
    )(lengths, *arrays)


def solution(mesh):
    placed = (
        P("ep", None),
        P(),
        P(None, "tp"),
        P(None, "tp"),
        P("tp", None, None),
        P(("ep", "tp"), None, None),
        P(("ep", "tp"), None, None),
        P(("ep", "tp")),
        P("tp", None, None),
        P("tp", None),
        P(),
        P(),
        P(),
        P(),
        P("ep", None, "tp"),
        P("ep", None, "tp"),
        P("ep", "tp", None),
        P(),
    )
    return jax.shard_map(
        body, mesh=mesh, in_specs=placed, out_specs=P(("ep", "tp"), None), check_vma=False
    )
```
